32 devices in a mesh: sp: 8 (over z, x), tp: 4 (over y, core).
Axes of the slice: x: 2, y: 2, z: 4, core: 2. Of those that a mesh axis runs over, the one named last changes fastest.
Arguments:
- tokens: bfloat16 [3072, 2048], P('sp'), may hold values from -6 to 6
- doc_ids: int32 [3072], P('sp'), may hold values from 0 to 2, never falling along the last dimension, each value on 1 to 2048 neighbouring positions
- pre_gain: float32 [2, 2048], replicated, may hold values from 0.1 to 1.9
- value_proj: bfloat16 [2, 2048, 1024], P(None, 'sp', 'tp'), may hold values from -0.1875 to 0.1875
- gate_proj: bfloat16 [2, 2048, 1024], P(None, 'sp', 'tp'), may hold values from -0.1875 to 0.1875
- out_proj: bfloat16 [2, 1024, 2048], P(None, 'tp', 'sp'), may hold values from -0.1875 to 0.1875
- conv_taps: float32 [2, 31, 1024], P(None, None, 'tp'), may hold values from -2.2 to 2.2
- norm_gain: float32 [2, 1024], P(None, 'tp'), may hold values from 0.1 to 1.9
- norm_shift: float32 [2, 1024], P(None, 'tp'), may hold values from -3 to 3
Outputs:
- hidden: bfloat16 [3072, 2048], P('sp')
The draws below stay inside these ranges and needn't reach their ends.
Inputs may be any that keep to these rules, and one draw needn't show every extreme that they name: `doc_ids`: document numbers never fall along the sequence; each document has 1 to 2048 positions.
All inputs are finite; a program needn't handle non-finite values.
Results may differ from the reference program's by a relative error of at most 0.017.
Values may be sent and summed in bfloat16 or wider, within the bound.
A program may use at most 64 MiB of HBM per device.

```python
import math
import jax
import jax.numpy as jnp
import numpy as np
from jax import lax

D = 2048
C = 1024
KW = 31
LAYERS = 2
TOKENS = 3072
DOCS = 3
DOC_MOST = 2048
N_TP = 4


def draw_conv_taps(key, part):
    scale_key = jax.random.fold_in(key, 11)
    tap_key = jax.random.fold_in(key, 12)
    group_scale = jnp.exp(jax.random.uniform(scale_key, (8,), jnp.float32, jnp.log(0.25), jnp.log(4.0)))
    channel_scale = jnp.repeat(group_scale, C // 8)
    raw = jnp.clip(jax.random.normal(tap_key, (LAYERS, KW, C), jnp.float32), -3.0, 3.0)
    return raw * channel_scale[None, None, :] / jnp.sqrt(jnp.float32(KW))


def spiked(drawn, stream_key, source, target, parts, factor):
    owner, partner = [(jnp.arange(drawn.shape[dim]) // (drawn.shape[dim] // parts)).reshape([-1 if axis == dim else 1 for axis in range(drawn.ndim)]) for dim in (source, target)]
    chosen = jax.random.permutation(stream_key, parts)[partner]
    strong = (owner == chosen) | (owner == (partner + parts // 2) % parts)
    return jnp.where(strong, factor * drawn, drawn)


def levels(rng, dims, shards, smallest, high):
    factor_of, own = 1.0, jax.random.fold_in(rng, 6)
    for dim, parts in shards:
        heights = jnp.exp(jax.random.uniform(jax.random.fold_in(own, dim), (parts,), jnp.float32, smallest / len(shards), high / len(shards)))
        factor_of = factor_of * jnp.repeat(heights, dims[dim] // parts).reshape([-1 if axis == dim else 1 for axis in range(len(dims))])
    return factor_of


def length_profile(count, total, most, lean):
    portions = [(1 << 20) // math.isqrt(rank ** lean) + 1 for rank in range(2, count + 1)]
    rest, holding = total - most - (count - 1), [1] * (count - 1)
    while rest > 0:
        movable = [i for i in range(count - 1) if holding[i] < most]
        whole, remaining = sum([portions[i] for i in movable]), rest
        for i in movable:
            extra = min(most - holding[i], max(1, remaining * portions[i] // whole), rest)
            holding[i] = holding[i] + extra
            rest = rest - extra
    return np.array([most] + holding)


def ragged_sizes(own_key, number_of, total, limit, slope):
    if number_of == 2:
        one = jax.random.randint(own_key, (), max(1, total - limit), min(limit, total - 1) + 1)
        return jnp.stack([one, total - one])
    sizes = jnp.asarray(length_profile(number_of, total, limit, slope), jnp.int32)
    couples = (number_of - 1) // 2
    giver, receiver = sizes[1:1 + 2 * couples:2], sizes[2:2 + 2 * couples:2]
    margin = jnp.minimum(giver - 1, limit - receiver)
    passed = jax.random.randint(jax.random.fold_in(own_key, 1), (couples,), 0, 1 << 20) % (margin + 1)
    sizes = sizes.at[1:1 + 2 * couples:2].set(giver - passed).at[2:2 + 2 * couples:2].set(receiver + passed)
    return sizes[jax.random.permutation(jax.random.fold_in(own_key, 2), number_of)]


def scatter_about(rng, extent, scale, most, cuts=(), held_as=jnp.bfloat16):
    array = scale * jax.random.normal(rng, extent, jnp.float32)
    if cuts:
        array = array * levels(rng, extent, cuts, -0.22, 0.18)
    return jnp.clip(array, -most, most).astype(held_as)


def gaussian_with(rng, dims, scale, limit, cuts, heavy, dtype=jnp.bfloat16):
    array = scale * jax.random.normal(rng, dims, jnp.float32)
    if cuts:
        array = array * levels(rng, dims, cuts, -0.22, 0.18)
    return jnp.clip(spiked(array, jax.random.fold_in(rng, 3), *heavy), -limit, limit).astype(dtype)


def setup_inputs(seed: int = 0) -> dict:
    seeds = jax.random.split(jax.random.key(seed), 10)
    tokens = scatter_about(seeds[0], (TOKENS, D), 1.0, 6.0, ((0, 8),))
    doc_ids = jnp.searchsorted(jnp.cumsum(ragged_sizes(seeds[1], DOCS, TOKENS, DOC_MOST, 0)), jnp.arange(TOKENS), side="right").astype(jnp.int32)
    pre_gain = jnp.clip(1.0 + 0.18 * jax.random.normal(seeds[2], (LAYERS, D), jnp.float32), 0.1, 1.9)
    value_proj = gaussian_with(seeds[3], (LAYERS, D, C), D ** -0.5, 0.1875, ((1, 8), (2, 4)), (1, 2, 8, 2.0))
    gate_proj = gaussian_with(seeds[4], (LAYERS, D, C), D ** -0.5, 0.1875, ((1, 8), (2, 4)), (1, 2, 8, 2.0))
    out_proj = scatter_about(seeds[5], (LAYERS, C, D), C ** -0.5, 0.1875, ((1, 4), (2, 8)))
    conv_taps = draw_conv_taps(jax.random.fold_in(seeds[9], 71), 0)
    norm_gain = jnp.clip(1.0 + 0.18 * jax.random.normal(seeds[7], (LAYERS, C), jnp.float32), 0.1, 1.9)
    norm_shift = scatter_about(seeds[8], (LAYERS, C), 0.5, 3.0, ((1, 4),), jnp.float32)
    return dict(tokens=tokens, doc_ids=doc_ids, pre_gain=pre_gain, value_proj=value_proj, gate_proj=gate_proj, out_proj=out_proj, conv_taps=conv_taps, norm_gain=norm_gain, norm_shift=norm_shift)


epsilon = 1e-06

def reference(tokens, doc_ids, pre_gain, value_proj, gate_proj, out_proj, conv_taps, norm_gain, norm_shift):
    hidden = tokens
    padded_docs = jnp.concatenate([jnp.full((KW - 1,), -1, jnp.int32), doc_ids.astype(jnp.int32)])
    block_width = C // N_TP
    for layer_index in range(LAYERS):
        wide_state = hidden.astype(jnp.float32)
        scale = lax.rsqrt(lax.optimization_barrier(jnp.mean(wide_state * wide_state, axis=-1, keepdims=True)) + epsilon)
        normed = (wide_state * scale * pre_gain[layer_index]).astype(jnp.bfloat16)
        value_half = jnp.dot(normed, value_proj[layer_index], preferred_element_type=jnp.float32).astype(jnp.bfloat16)
        gate_half = jnp.dot(normed, gate_proj[layer_index], preferred_element_type=jnp.float32).astype(jnp.bfloat16)
        gated_rows = (value_half.astype(jnp.float32) * jax.nn.sigmoid(gate_half.astype(jnp.float32))).astype(jnp.bfloat16)
        padded = jnp.concatenate([jnp.zeros((KW - 1, C), jnp.bfloat16), gated_rows]).astype(jnp.float32)
        conv_out = jnp.zeros((TOKENS, C), jnp.float32)
        for offset in range(KW):
            first_row = KW - 1 - offset
            same_doc = (padded_docs[first_row:first_row + TOKENS] == doc_ids)[:, None]
            term = conv_taps[layer_index, offset][None, :] * padded[first_row:first_row + TOKENS]
            conv_out = conv_out + jnp.where(same_doc, term, jnp.float32(0.0))
        row_mean = lax.optimization_barrier(jnp.mean(conv_out, axis=-1, keepdims=True))
        row_var = lax.optimization_barrier(jnp.mean(jnp.square(conv_out - row_mean), axis=-1, keepdims=True))
        normalized = norm_gain[layer_index] * (conv_out - row_mean) * lax.rsqrt(row_var + epsilon) + norm_shift[layer_index]
        activated = jax.nn.silu(normalized).astype(jnp.bfloat16)
        total = jnp.zeros((TOKENS, D), jnp.float32)
        for block_index in range(N_TP):
            lower = block_index * block_width
            share = jnp.dot(activated[:, lower:lower + block_width], out_proj[layer_index, lower:lower + block_width], preferred_element_type=jnp.float32)
            total = total + share.astype(jnp.bfloat16).astype(jnp.float32)
        branch = total.astype(jnp.bfloat16)
        hidden = (hidden.astype(jnp.float32) + branch.astype(jnp.float32)).astype(jnp.bfloat16)
    return hidden
```

```python
import functools
import jax
import jax.numpy as jnp
from jax import lax
from jax.experimental import pallas as pl
from jax.experimental.pallas import tpu as pltpu
from jax.sharding import PartitionSpec as P

epsilon = 1e-06
MESH = pl.DeviceIdType.MESH
HALO = 32
CONV_ROWS = 64


def fused_kernel(
    n, m, reach, layers,
    tok_ref, doc_ref, gain_ref, v_ref, g_ref, o_ref, tap_ref, ng_ref, ns_ref,
    out_ref,
    w, oring, ofull, normed, acc, padded, pdoc, run, ghalo, halo_in, doc_in,
    stat, stat_out, stat_in, conv, act_all, hid,
    rsend, rrecv, osend, orecv, hsend, hrecv, ssend, srecv, asend, arecv, xsend, xrecv,
):
    me = lax.axis_index("sp")
    t = lax.axis_index("tp")
    q, c = t // 2, t % 2
    pairs = m // 2
    half_n = n // 2
    rows, width = tok_ref.shape
    depth, block = v_ref.shape[1], v_ref.shape[2]
    owidth = o_ref.shape[2]
    hd, ho = depth // 2, owidth // 2
    half_width = width // 2
    channels = block * m

    def index_of(position):
        position = (position + 2 * n) % n
        return jnp.where(position < half_n, 2 * position, 2 * (n - 1 - position) + 1)

    my_pos = jnp.where(me % 2 == 0, me // 2, n - 1 - me // 2)
    right, left = index_of(my_pos + 1), index_of(my_pos - 1)
    following, before = (me + 1) % n, (me + n - 1) % n

    barrier = pltpu.get_barrier_semaphore()
    for other in (right, left, following, before):
        pl.semaphore_signal(barrier, inc=1, device_id={"sp": other}, device_id_type=MESH)
    for k in range(1, m):
        pl.semaphore_signal(barrier, inc=1, device_id={"tp": (t + k) % m}, device_id_type=MESH)
    pl.semaphore_wait(barrier, 3 + m)

    def to_sp(src, dst, send, recv, target):
        return pltpu.make_async_remote_copy(
            src_ref=src, dst_ref=dst, send_sem=send, recv_sem=recv,
            device_id={"sp": target}, device_id_type=MESH)

    def to_tp(src, dst, send, recv, target):
        return pltpu.make_async_remote_copy(
            src_ref=src, dst_ref=dst, send_sem=send, recv_sem=recv,
            device_id={"tp": target}, device_id_type=MESH)

    def w_piece(layer, owner, way, part):
        return w.at[layer, pl.ds(pl.multiple_of(owner * depth + part * hd, hd), hd),
                    pl.ds(way * block, block)]

    def o_piece(layer, owner, way):
        return oring.at[layer, :, pl.ds(pl.multiple_of(owner * owidth + way * ho, ho), ho)]

    def ring_copy(layer, msg, way, step, own=False):
        owner = index_of(my_pos - step if way == 0 else my_pos + step)
        if msg < 2:
            dst = w_piece(layer, owner, way, msg)
            src = (v_ref, g_ref)[way].at[layer, pl.ds(msg * hd, hd), :] if own else dst
        else:
            dst = o_piece(layer, owner, way)
            src = o_ref.at[layer, :, pl.ds(way * ho, ho)] if own else dst
        return to_sp(src, dst, rsend.at[layer, msg, way, step], rrecv.at[layer, msg, way, step],
                     right if way == 0 else left)

    def arrival(layer, msg, way, step):
        owner = index_of(my_pos - step - 1 if way == 0 else my_pos + step + 1)
        dst = w_piece(layer, owner, way, msg) if msg < 2 else o_piece(layer, owner, way)
        return to_sp(dst, dst, rsend.at[layer, msg, way, step], rrecv.at[layer, msg, way, step],
                     right if way == 0 else left)

    def spread_copy(layer, way, step, pair, own=False):
        owner = index_of(my_pos - step if way == 0 else my_pos + step)
        part = owner // half_n
        local = owner - part * half_n
        src = o_ref.at[layer, :, pl.ds(way * ho, ho)] if own else o_piece(layer, owner, way)
        dst = ofull.at[layer, pl.ds(pl.multiple_of(t * block, block), block),
                       pl.ds(pl.multiple_of(local * owidth + way * ho, ho), ho)]
        copy = to_tp(src, dst, osend.at[layer, way, step, pair],
                     orecv.at[layer, t, local * 2 + way], 2 * ((q + pair) % pairs) + part)
        return copy, part

    def spread(layer, way, step, act, own=False):
        for pair in range(pairs - 1, -1, -1):
            copy, part = spread_copy(layer, way, step, pair, own)
            if pair == 0:
                pl.when(part != c)(lambda copy=copy: getattr(copy, act)())
            else:
                getattr(copy, act)()

    def open_ring(layer):
        for msg in range(3):
            for way in range(2):
                ring_copy(layer, msg, way, 0, own=True).start()
        for way in range(2):
            spread(layer, way, 0, "start", own=True)

    def keep_own(layer):
        row = pl.ds(pl.multiple_of(me * depth, depth), depth)
        w[layer, row, pl.ds(0, block)] = v_ref[layer]
        w[layer, row, pl.ds(block, block)] = g_ref[layer]
        oring[layer, :, pl.ds(pl.multiple_of(me * owidth, owidth), owidth)] = o_ref[layer]

    def service(layer, first, last):
        @pl.loop(first, last)
        def _(step):
            for msg in range(3):
                for way in range(2):
                    arrival(layer, msg, way, step - 1).wait_recv()
                    ring_copy(layer, msg, way, step).start()
            for way in range(2):
                spread(layer, way, step, "start")

    def finish_ring(layer):
        for msg in range(3):
            for way in range(2):
                arrival(layer, msg, way, n - 2).wait_recv()
        for way in range(2):
            spread(layer, way, n - 1, "start")

    open_ring(0)
    doc_copy = to_sp(doc_ref.at[pl.ds(rows - HALO, HALO), :], doc_in, hsend.at[layers],
                     hrecv.at[layers], following)
    doc_copy.start()

    def norm_rows(layer, source):
        @pl.loop(0, rows // 32)
        def _(i):
            span = pl.ds(pl.multiple_of(i * 32, 32), 32)
            wide = source[span, :].astype(jnp.float32)
            scale = lax.rsqrt(jnp.mean(wide * wide, axis=-1, keepdims=True) + epsilon)
            normed[span, :] = (wide * scale * gain_ref[pl.ds(layer, 1), :]).astype(jnp.bfloat16)

    norm_rows(0, tok_ref)
    keep_own(0)
    service(0, 1, 2)
    doc_copy.wait_recv()
    pdoc[pl.ds(0, HALO), :] = jnp.where(me == 0, -1, doc_in[...])
    pdoc[pl.ds(HALO, rows), :] = doc_ref[...]

    @pl.loop(0, rows // CONV_ROWS)
    def _(i):
        base = pl.multiple_of(i * CONV_ROWS, CONV_ROWS)
        mine = pdoc[pl.ds(base + HALO, CONV_ROWS), :]
        count = jnp.zeros_like(mine)
        for j in range(1, reach + 1):
            count = count + (pdoc[pl.ds(base + (HALO - j), CONV_ROWS), :] == mine).astype(jnp.int32)
        run[pl.ds(base, CONV_ROWS), :] = count

    service(0, 2, n - 1)
    if layers > 1:
        for later in range(1, layers):
            keep_own(later)

    lane = lax.broadcasted_iota(jnp.int32, (CONV_ROWS, 128), 1)

    def layer_step(layer, source, target):
        nxt = layer + 1 if layer + 1 < layers else None
        marks = iter([(1, 2), (2, 3), (3, 4), (4, 5), (5, 6), (6, n - 1)] if n == 8 else [(1, n - 1)])

        def tend():
            if nxt is not None:
                span = next(marks, None)
                if span is not None:
                    service(nxt, *span)

        if nxt is not None:
            open_ring(nxt)
        finish_ring(layer)
        acc[...] = jnp.dot(normed[...], w[layer], preferred_element_type=jnp.float32)

        def store_padded(row, values):
            for part in range(block // 128):
                padded[pl.ds(row + part * (rows + HALO), 32), :] = values[:, part * 128:(part + 1) * 128].astype(jnp.float32)

        def gate_rows(i):
            span = pl.ds(pl.multiple_of(i * 32, 32), 32)
            value = acc[span, pl.ds(0, block)].astype(jnp.bfloat16).astype(jnp.float32)
            gate = acc[span, pl.ds(block, block)].astype(jnp.bfloat16).astype(jnp.float32)
            gated = (value * jax.nn.sigmoid(gate)).astype(jnp.bfloat16)
            store_padded(pl.multiple_of(i * 32 + HALO, 32), gated)
            return gated

        ghalo[layer] = gate_rows(rows // 32 - 1)
        halo_copy = to_sp(ghalo.at[layer], halo_in.at[layer], hsend.at[layer], hrecv.at[layer], following)
        halo_copy.start()

        @pl.loop(0, rows // 32 - 1)
        def _(i):
            gate_rows(i)

        tend()
        halo_copy.wait_recv()
        store_padded(0, halo_in[layer])

        @pl.loop(0, rows // CONV_ROWS)
        def _(i):
            base = pl.multiple_of(i * CONV_ROWS, CONV_ROWS)
            count = run[pl.ds(base, CONV_ROWS), :]
            first_sum = jnp.zeros((CONV_ROWS, 1), jnp.float32)
            square_sum = jnp.zeros((CONV_ROWS, 1), jnp.float32)
            for part in range(block // 128):
                cols = pl.ds(part * 128, 128)
                lift = part * (rows + HALO)
                total = tap_ref[layer, pl.ds(0, 1), cols] * padded[pl.ds(base + (lift + HALO), CONV_ROWS), :]
                for j in range(1, reach + 1):
                    term = tap_ref[layer, pl.ds(j, 1), cols] * padded[pl.ds(base + (lift + HALO - j), CONV_ROWS), :]
                    total = total + jnp.where(count >= j, term, jnp.float32(0.0))
                conv[pl.ds(base, CONV_ROWS), cols] = total
                first_sum = first_sum + jnp.sum(total, axis=1, keepdims=True)
                square_sum = square_sum + jnp.sum(total * total, axis=1, keepdims=True)
            stat[pl.ds(base, CONV_ROWS), :] = jnp.where(
                lane == 0, first_sum, jnp.where(lane == 1, square_sum, jnp.float32(0.0)))

        stat_out[layer] = jnp.transpose(stat[...])[:8]
        stat_copies = [
            to_tp(stat_out.at[layer], stat_in.at[layer, t], ssend.at[layer, k], srecv.at[layer, t], (t + k) % m)
            for k in range(1, m)]
        for copy in stat_copies:
            copy.start()
        tend()
        summed = stat_out[layer]
        for k in range(1, m):
            peer = (t + k) % m
            to_tp(stat_in.at[layer, peer], stat_in.at[layer, peer], ssend.at[layer, k],
                  srecv.at[layer, peer], peer).wait_recv()
            summed = summed + stat_in[layer, peer]
        stat[...] = jnp.transpose(
            jnp.concatenate([summed, jnp.zeros((120, rows), jnp.float32)], axis=0))

        mine = pl.ds(pl.multiple_of(t * block, block), block)

        @pl.loop(0, rows // CONV_ROWS)
        def _(i):
            span = pl.ds(pl.multiple_of(i * CONV_ROWS, CONV_ROWS), CONV_ROWS)
            both = stat[span, :]
            row_mean = both[:, 0:1] / channels
            row_var = both[:, 1:2] / channels - row_mean * row_mean
            normalized = (ng_ref[pl.ds(layer, 1), :] * (conv[span, :] - row_mean)
                          * lax.rsqrt(row_var + epsilon) + ns_ref[pl.ds(layer, 1), :])
            act_all[layer, span, mine] = jax.nn.silu(normalized).astype(jnp.bfloat16)

        def act_cols(who):
            return act_all.at[layer, :, pl.ds(pl.multiple_of(who * block, block), block)]

        partner = 2 * q + 1 - c
        copies = []
        for k in range(pairs - 1, -1, -1):
            target_t = 2 * ((q + k) % pairs) + c if k else partner
            copies.append(to_tp(act_cols(t), act_cols(t), asend.at[layer, k], arecv.at[layer, t], target_t))
            copies[-1].start()
        tend()
        for k in range(1, pairs):
            sender = 2 * ((q + k) % pairs) + c
            to_tp(act_cols(sender), act_cols(sender), asend.at[layer, k], arecv.at[layer, sender], sender).wait_recv()
            copies.append(to_tp(act_cols(sender), act_cols(sender), asend.at[layer, pairs + k],
                                arecv.at[layer, sender], partner))
            copies[-1].start()
        tend()
        ofull[layer, pl.ds(pl.multiple_of(t * block, block), block), :] = oring[
            layer, :, pl.ds(pl.multiple_of(c * half_width, half_width), half_width)]
        for k in range(1, m):
            peer = (t + k) % m

            @pl.loop(0, n)
            def _(piece, peer=peer):
                dst = ofull.at[layer, pl.ds(pl.multiple_of(peer * block, block), block),
                               pl.ds(pl.multiple_of(piece * ho, ho), ho)]
                to_tp(dst, dst, osend.at[layer, 0, 0, 0], orecv.at[layer, peer, piece], peer).wait_recv()

        for k in range(pairs):
            sender = 2 * ((q + k) % pairs) + 1 - c
            to_tp(act_cols(sender), act_cols(sender), asend.at[layer, k], arecv.at[layer, sender], partner).wait_recv()
        half = pl.ds(pl.multiple_of(c * half_width, half_width), half_width)
        branch = jnp.dot(act_all[layer], ofull[layer], preferred_element_type=jnp.float32).astype(jnp.bfloat16)
        target[:, half] = (source[:, half].astype(jnp.float32) + branch.astype(jnp.float32)).astype(jnp.bfloat16)
        swap = to_tp(target.at[:, half], target.at[:, half], xsend.at[layer], xrecv.at[layer], partner)
        swap.start()
        tend()
        swap.wait_recv()
        tend()
        if nxt is not None:
            norm_rows(nxt, target)
        tend()
        for copy in copies + stat_copies + [halo_copy]:
            copy.wait_send()
        swap.wait_send()

    for layer in range(layers):
        layer_step(layer, tok_ref if layer == 0 else hid.at[layer - 1], hid.at[layer])
    out_ref[...] = hid[layers - 1]

    doc_copy.wait_send()

    @pl.loop(0, n - 1)
    def _(step):
        for layer in range(layers):
            for msg in range(3):
                for way in range(2):
                    ring_copy(layer, msg, way, step).wait_send()

    @pl.loop(0, n)
    def _(step):
        for layer in range(layers):
            for way in range(2):
                spread(layer, way, step, "wait_send")


def fused_on_device(n, m, tokens, doc_ids, pre_gain, value_proj, gate_proj, out_proj, conv_taps, norm_gain, norm_shift):
    rows, width = tokens.shape
    layers, depth, block = value_proj.shape
    owidth = out_proj.shape[2]
    reach = conv_taps.shape[1] - 1
    channels = block * m
    docs = jnp.broadcast_to(doc_ids[:, None], (rows, 128))
    bf16, f32, i32 = jnp.bfloat16, jnp.float32, jnp.int32
    dma = pltpu.SemaphoreType.DMA
    vmem = pl.BlockSpec(memory_space=pltpu.VMEM)
    return pl.pallas_call(
        functools.partial(fused_kernel, n, m, reach, layers),
        out_shape=jax.ShapeDtypeStruct((rows, width), bf16),
        in_specs=[vmem] * 9,
        out_specs=vmem,
        scratch_shapes=[
            pltpu.VMEM((layers, n * depth, 2 * block), bf16),
            pltpu.VMEM((layers, block, n * owidth), bf16),
            pltpu.VMEM((layers, channels, width // 2), bf16),
            pltpu.VMEM((rows, width), bf16),
            pltpu.VMEM((rows, 2 * block), f32),
            pltpu.VMEM((block // 128 * (rows + HALO), 128), f32),
            pltpu.VMEM((rows + HALO, 128), i32),
            pltpu.VMEM((rows, 128), i32),
            pltpu.VMEM((layers, HALO, block), bf16),
            pltpu.VMEM((layers, HALO, block), bf16),
            pltpu.VMEM((HALO, 128), i32),
            pltpu.VMEM((rows, 128), f32),
            pltpu.VMEM((layers, 8, rows), f32),
            pltpu.VMEM((layers, m, 8, rows), f32),
            pltpu.VMEM((rows, block), f32),
            pltpu.VMEM((layers, rows, channels), bf16),
            pltpu.VMEM((layers, rows, width), bf16),
            dma((layers, 3, 2, n)), dma((layers, 3, 2, n)),
            dma((layers, 2, n, m // 2)), dma((layers, m, n)),
            dma((layers + 1,)), dma((layers + 1,)),
            dma((layers, m)), dma((layers, m)),
            dma((layers, m)), dma((layers, m)),
            dma((layers,)), dma((layers,)),
        ],
        compiler_params=pltpu.CompilerParams(
            collective_id=0, has_side_effects=True, vmem_limit_bytes=60 * 1024 * 1024),
    )(tokens, docs, pre_gain, value_proj, gate_proj, out_proj, conv_taps, norm_gain, norm_shift)


def passed_along(value, axis, steps):
    count = lax.axis_size(axis)
    first, last = (max(0, -steps), min(count, count - steps))
    return lax.ppermute(value, axis, [(source, source + steps) for source in range(first, last)])


def on_device(
    tokens, doc_ids, pre_gain, value_proj, gate_proj, out_proj, conv_taps, norm_gain, norm_shift
):
    layer_count = value_proj.shape[0]
    tap_count = conv_taps.shape[1]
    reach_rows = tap_count - 1
    row_count = tokens.shape[0]
    block_width = conv_taps.shape[2]
    channels = block_width * lax.axis_size("tp")
    hidden = tokens
    full_value, full_gate, full_out = (
        lax.all_gather(value_proj, "sp", axis=1, tiled=True),
        lax.all_gather(gate_proj, "sp", axis=1, tiled=True),
        lax.all_gather(out_proj, "sp", axis=2, tiled=True),
    )
    for layer_index in range(layer_count):
        wide_state = hidden.astype(jnp.float32)
        scale = lax.rsqrt(jnp.mean(wide_state * wide_state, axis=-1, keepdims=True) + epsilon)
        normed = (wide_state * scale * pre_gain[layer_index]).astype(jnp.bfloat16)
        value_acc = jnp.dot(normed, full_value[layer_index], preferred_element_type=jnp.float32)
        gate_acc = jnp.dot(normed, full_gate[layer_index], preferred_element_type=jnp.float32)
        value_half = value_acc.astype(jnp.bfloat16)
        gate_half = gate_acc.astype(jnp.bfloat16)
        gated_rows = (
            value_half.astype(jnp.float32) * jax.nn.sigmoid(gate_half.astype(jnp.float32))
        ).astype(jnp.bfloat16)
        prev_rows, prev_docs = passed_along(
            (gated_rows[row_count - reach_rows :], doc_ids[row_count - reach_rows :]), "sp", 1
        )
        padded = jnp.concatenate([prev_rows, gated_rows]).astype(jnp.float32)
        padded_docs = jnp.concatenate([prev_docs, doc_ids])
        conv_out = jnp.zeros((row_count, block_width), jnp.float32)
        for offset in range(tap_count):
            first_row = reach_rows - offset
            same_doc = (padded_docs[first_row : first_row + row_count] == doc_ids)[:, None]
            term = (
                conv_taps[layer_index, offset][None, :] * padded[first_row : first_row + row_count]
            )
            conv_out = conv_out + jnp.where(same_doc, term, jnp.float32(0.0))
        row_sums, square_sums = lax.psum(
            (jnp.sum(conv_out, axis=1), jnp.sum(conv_out * conv_out, axis=1)), "tp"
        )
        row_mean = (row_sums / channels)[:, None]
        row_var = (square_sums / channels)[:, None] - row_mean * row_mean
        normalized = (
            norm_gain[layer_index] * (conv_out - row_mean) * lax.rsqrt(row_var + epsilon)
            + norm_shift[layer_index]
        )
        activated = jax.nn.silu(normalized).astype(jnp.bfloat16)
        partial_value = jnp.dot(
            activated, full_out[layer_index], preferred_element_type=jnp.float32
        )
        summed = lax.psum(partial_value.astype(jnp.bfloat16), "tp")
        hidden = (hidden.astype(jnp.float32) + summed.astype(jnp.float32)).astype(jnp.bfloat16)
    return hidden


def suits_kernel(n, m, tokens, value_proj, out_proj, conv_taps):
    rows, width = tokens.shape
    depth, block = value_proj.shape[1:]
    return (
        n % 2 == 0 and 4 <= n <= 16 and m % 2 == 0 and m >= 4 and rows % 128 == 0 and width % 256 == 0
        and depth % 32 == 0 and block % 128 == 0 and out_proj.shape[2] % 256 == 0
        and conv_taps.shape[1] - 1 <= HALO
    )


def solution(mesh):
    n, m = mesh.shape["sp"], mesh.shape["tp"]

    def body(tokens, doc_ids, pre_gain, value_proj, gate_proj, out_proj, conv_taps, norm_gain, norm_shift):
        chosen = on_device
        if suits_kernel(n, m, tokens, value_proj, out_proj, conv_taps):
            chosen = functools.partial(fused_on_device, n, m)
        return chosen(tokens, doc_ids, pre_gain, value_proj, gate_proj, out_proj, conv_taps, norm_gain, norm_shift)

    return jax.shard_map(
        body,
        mesh=mesh,
        in_specs=(
            P("sp", None),
            P("sp"),
            P(),
            P(None, "sp", "tp"),
            P(None, "sp", "tp"),
            P(None, "tp", "sp"),
            P(None, None, "tp"),
            P(None, "tp"),
            P(None, "tp"),
        ),
        out_specs=P("sp", None),
        check_vma=False,
    )
```

```python
import functools
import jax
import jax.numpy as jnp
from jax import lax
from jax.experimental import pallas as pl
from jax.experimental.pallas import tpu as pltpu
from jax.sharding import PartitionSpec as P

epsilon = 1e-06
MESH = pl.DeviceIdType.MESH
HALO = 32
CONV_ROWS = 64


def fused_kernel(
    n, m, reach, layers,
    tok_ref, doc_ref, gain_ref, v_ref, g_ref, o_ref, tap_ref, ng_ref, ns_ref,
    out_ref,
    w, oring, ofull, normed, acc, padded, pdoc, run, ghalo, halo_in, doc_in, doc_tail,
    stat, stat_out, stat_in, conv, act_all, hid,
    rsend, rrecv, osend, orecv, hsend, hrecv, ssend, srecv, asend, arecv, xsend, xrecv,
):
    me = lax.axis_index("sp")
    t = lax.axis_index("tp")
    q, c = t // 2, t % 2
    pairs = m // 2
    half_n = n // 2
    rows, width = tok_ref.shape
    depth, block = v_ref.shape[1], v_ref.shape[2]
    owidth = o_ref.shape[2]
    hd, ho = depth // 2, owidth // 2
    half_width = width // 2
    channels = block * m

    def index_of(position):
        position = (position + 2 * n) % n
        return jnp.where(position < half_n, 2 * position, 2 * (n - 1 - position) + 1)

    my_pos = jnp.where(me % 2 == 0, me // 2, n - 1 - me // 2)
    right, left = index_of(my_pos + 1), index_of(my_pos - 1)
    following, before = (me + 1) % n, (me + n - 1) % n

    barrier = pltpu.get_barrier_semaphore()
    for other in (right, left, following, before):
        pl.semaphore_signal(barrier, inc=1, device_id={"sp": other}, device_id_type=MESH)
    for k in range(1, m):
        pl.semaphore_signal(barrier, inc=1, device_id={"tp": (t + k) % m}, device_id_type=MESH)
    pl.semaphore_wait(barrier, 3 + m)

    def to_sp(src, dst, send, recv, target):
        return pltpu.make_async_remote_copy(
            src_ref=src, dst_ref=dst, send_sem=send, recv_sem=recv,
            device_id={"sp": target}, device_id_type=MESH)

    def to_tp(src, dst, send, recv, target):
        return pltpu.make_async_remote_copy(
            src_ref=src, dst_ref=dst, send_sem=send, recv_sem=recv,
            device_id={"tp": target}, device_id_type=MESH)

    def w_piece(layer, owner, way, part):
        return w.at[layer, pl.ds(pl.multiple_of(owner * depth + part * hd, hd), hd),
                    pl.ds(way * block, block)]

    def o_piece(layer, owner, way):
        return oring.at[layer, :, pl.ds(pl.multiple_of(owner * owidth + way * ho, ho), ho)]

    def ring_copy(layer, msg, way, step, own=False):
        owner = index_of(my_pos - step if way == 0 else my_pos + step)
        if msg < 2:
            dst = w_piece(layer, owner, way, msg)
            src = (v_ref, g_ref)[way].at[layer, pl.ds(msg * hd, hd), :] if own else dst
        else:
            dst = o_piece(layer, owner, way)
            src = o_ref.at[layer, :, pl.ds(way * ho, ho)] if own else dst
        return to_sp(src, dst, rsend.at[layer, msg, way, step], rrecv.at[layer, msg, way, step],
                     right if way == 0 else left)

    def arrival(layer, msg, way, step):
        owner = index_of(my_pos - step - 1 if way == 0 else my_pos + step + 1)
        dst = w_piece(layer, owner, way, msg) if msg < 2 else o_piece(layer, owner, way)
        return to_sp(dst, dst, rsend.at[layer, msg, way, step], rrecv.at[layer, msg, way, step],
                     right if way == 0 else left)

    def spread_copy(layer, way, step, pair, own=False):
        owner = index_of(my_pos - step if way == 0 else my_pos + step)
        part = owner // half_n
        local = owner - part * half_n
        src = o_ref.at[layer, :, pl.ds(way * ho, ho)] if own else o_piece(layer, owner, way)
        dst = ofull.at[layer, pl.ds(pl.multiple_of(t * block, block), block),
                       pl.ds(pl.multiple_of(local * owidth + way * ho, ho), ho)]
        copy = to_tp(src, dst, osend.at[layer, way, step, pair],
                     orecv.at[layer, t, local * 2 + way], 2 * ((q + pair) % pairs) + part)
        return copy, part

    def spread(layer, way, step, act, own=False):
        for pair in range(pairs - 1, -1, -1):
            copy, part = spread_copy(layer, way, step, pair, own)
            if pair == 0:
                pl.when(part != c)(lambda copy=copy: getattr(copy, act)())
            else:
                getattr(copy, act)()

    def stream(layer, step, msgs):
        for way in range(2):
            if step > 0:
                for msg in msgs:
                    arrival(layer, msg, way, step - 1).wait_recv()
                    if step < n - 1:
                        ring_copy(layer, msg, way, step).start()
            else:
                for msg in msgs:
                    ring_copy(layer, msg, way, 0, own=True).start()
            if 2 in msgs:
                spread(layer, way, step, "start", own=step == 0)

    lag = min(3, n - 1)

    def slot(time):
        for layer in range(layers):
            for msgs, late in (((0, 1), 0), ((2,), lag)):
                step = time - (n - 1) * layer - late
                if 0 <= step <= n - 1:
                    stream(layer, step, msgs)

    def keep_own(layer):
        row = pl.ds(pl.multiple_of(me * depth, depth), depth)
        w[layer, row, pl.ds(0, block)] = v_ref[layer]
        w[layer, row, pl.ds(block, block)] = g_ref[layer]
        oring[layer, :, pl.ds(pl.multiple_of(me * owidth, owidth), owidth)] = o_ref[layer]

    slot(0)

    def doc_block(i):
        row = doc_ref[pl.ds(i, 1), :].astype(jnp.float32)
        return jnp.transpose(jnp.broadcast_to(row, (128, 128)))

    doc_tail[...] = doc_block(rows // 128 - 1)[128 - HALO:]
    doc_copy = to_sp(doc_tail, doc_in, hsend.at[layers],
                     hrecv.at[layers], following)
    doc_copy.start()

    for i in range(rows // 128):
        pdoc[pl.ds(HALO + i * 128, 128), :] = doc_block(i)

    def norm_rows(layer, source):
        @pl.loop(0, rows // 32)
        def _(i):
            span = pl.ds(pl.multiple_of(i * 32, 32), 32)
            wide = source[span, :].astype(jnp.float32)
            scale = lax.rsqrt(jnp.mean(wide * wide, axis=-1, keepdims=True) + epsilon)
            normed[span, :] = (wide * scale * gain_ref[pl.ds(layer, 1), :]).astype(jnp.bfloat16)

    norm_rows(0, tok_ref)
    keep_own(0)
    slot(1)
    doc_copy.wait_recv()
    pdoc[pl.ds(0, HALO), :] = jnp.where(me == 0, jnp.float32(-1.0), doc_in[...])

    @pl.loop(0, rows // CONV_ROWS)
    def _(i):
        base = pl.multiple_of(i * CONV_ROWS, CONV_ROWS)
        mine = pdoc[pl.ds(base + HALO, CONV_ROWS), :]
        count = jnp.zeros((CONV_ROWS, 128), jnp.int32)
        for j in range(1, reach + 1):
            count = count + (pdoc[pl.ds(base + (HALO - j), CONV_ROWS), :] == mine).astype(jnp.int32)
        run[pl.ds(base, CONV_ROWS), :] = count

    for later in range(1, layers):
        keep_own(later)
    for time in range(2, n):
        slot(time)

    lane = lax.broadcasted_iota(jnp.int32, (CONV_ROWS, 128), 1)

    def layer_step(layer, source, target):
        nxt = layer + 1 if layer + 1 < layers else None
        opened = (n - 1) * (layer + 1) + 1
        times = list(range(opened, opened + (n - 1 if nxt is not None else lag)))
        shares = [times[i:i + 1] for i in range(6)] + [times[6:]]

        def tend():
            for time in shares.pop(0):
                slot(time)

        acc[...] = jnp.dot(normed[...], w[layer], preferred_element_type=jnp.float32)

        def store_padded(row, values):
            for part in range(block // 128):
                padded[pl.ds(row + part * (rows + HALO), 32), :] = values[:, part * 128:(part + 1) * 128].astype(jnp.float32)

        def gate_rows(i):
            span = pl.ds(pl.multiple_of(i * 32, 32), 32)
            value = acc[span, pl.ds(0, block)].astype(jnp.bfloat16).astype(jnp.float32)
            gate = acc[span, pl.ds(block, block)].astype(jnp.bfloat16).astype(jnp.float32)
            gated = (value * jax.nn.sigmoid(gate)).astype(jnp.bfloat16)
            store_padded(pl.multiple_of(i * 32 + HALO, 32), gated)
            return gated

        ghalo[layer] = gate_rows(rows // 32 - 1)
        halo_copy = to_sp(ghalo.at[layer], halo_in.at[layer], hsend.at[layer], hrecv.at[layer], following)
        halo_copy.start()

        @pl.loop(0, rows // 32 - 1)
        def _(i):
            gate_rows(i)

        tend()
        halo_copy.wait_recv()
        store_padded(0, halo_in[layer])

        @pl.loop(0, rows // CONV_ROWS)
        def _(i):
            base = pl.multiple_of(i * CONV_ROWS, CONV_ROWS)
            count = run[pl.ds(base, CONV_ROWS), :]
            first_sum = jnp.zeros((CONV_ROWS, 1), jnp.float32)
            square_sum = jnp.zeros((CONV_ROWS, 1), jnp.float32)
            for part in range(block // 128):
                cols = pl.ds(part * 128, 128)
                lift = part * (rows + HALO)
                total = tap_ref[0, pl.ds(layer, 1), cols] * padded[pl.ds(base + (lift + HALO), CONV_ROWS), :]
                for j in range(1, reach + 1):
                    term = tap_ref[j, pl.ds(layer, 1), cols] * padded[pl.ds(base + (lift + HALO - j), CONV_ROWS), :]
                    total = total + jnp.where(count >= j, term, jnp.float32(0.0))
                conv[pl.ds(base, CONV_ROWS), cols] = total
                first_sum = first_sum + jnp.sum(total, axis=1, keepdims=True)
                square_sum = square_sum + jnp.sum(total * total, axis=1, keepdims=True)
            stat[pl.ds(base, CONV_ROWS), :] = jnp.where(
                lane == 0, first_sum, jnp.where(lane == 1, square_sum, jnp.float32(0.0)))

        stat_out[layer] = jnp.transpose(stat[...])[:8]
        stat_copies = [
            to_tp(stat_out.at[layer], stat_in.at[layer, t], ssend.at[layer, k], srecv.at[layer, t], (t + k) % m)
            for k in range(1, m)]
        for copy in stat_copies:
            copy.start()
        tend()
        summed = stat_out[layer]
        for k in range(1, m):
            peer = (t + k) % m
            to_tp(stat_in.at[layer, peer], stat_in.at[layer, peer], ssend.at[layer, k],
                  srecv.at[layer, peer], peer).wait_recv()
            summed = summed + stat_in[layer, peer]
        stat[...] = jnp.transpose(
            jnp.concatenate([summed, jnp.zeros((120, rows), jnp.float32)], axis=0))

        mine = pl.ds(pl.multiple_of(t * block, block), block)

        @pl.loop(0, rows // CONV_ROWS)
        def _(i):
            span = pl.ds(pl.multiple_of(i * CONV_ROWS, CONV_ROWS), CONV_ROWS)
            both = stat[span, :]
            row_mean = both[:, 0:1] / channels
            row_var = both[:, 1:2] / channels - row_mean * row_mean
            normalized = (ng_ref[pl.ds(layer, 1), :] * (conv[span, :] - row_mean)
                          * lax.rsqrt(row_var + epsilon) + ns_ref[pl.ds(layer, 1), :])
            act_all[layer, span, mine] = jax.nn.silu(normalized).astype(jnp.bfloat16)

        def act_cols(who):
            return act_all.at[layer, :, pl.ds(pl.multiple_of(who * block, block), block)]

        partner = 2 * q + 1 - c
        copies = []
        for k in range(pairs - 1, -1, -1):
            target_t = 2 * ((q + k) % pairs) + c if k else partner
            copies.append(to_tp(act_cols(t), act_cols(t), asend.at[layer, k], arecv.at[layer, t], target_t))
            copies[-1].start()
        tend()
        for k in range(1, pairs):
            sender = 2 * ((q + k) % pairs) + c
            to_tp(act_cols(sender), act_cols(sender), asend.at[layer, k], arecv.at[layer, sender], sender).wait_recv()
            copies.append(to_tp(act_cols(sender), act_cols(sender), asend.at[layer, pairs + k],
                                arecv.at[layer, sender], partner))
            copies[-1].start()
        tend()
        ofull[layer, pl.ds(pl.multiple_of(t * block, block), block), :] = oring[
            layer, :, pl.ds(pl.multiple_of(c * half_width, half_width), half_width)]
        for k in range(1, m):
            peer = (t + k) % m

            @pl.loop(0, n)
            def _(piece, peer=peer):
                dst = ofull.at[layer, pl.ds(pl.multiple_of(peer * block, block), block),
                               pl.ds(pl.multiple_of(piece * ho, ho), ho)]
                to_tp(dst, dst, osend.at[layer, 0, 0, 0], orecv.at[layer, peer, piece], peer).wait_recv()

        for k in range(pairs):
            sender = 2 * ((q + k) % pairs) + 1 - c
            to_tp(act_cols(sender), act_cols(sender), asend.at[layer, k], arecv.at[layer, sender], partner).wait_recv()
        half = pl.ds(pl.multiple_of(c * half_width, half_width), half_width)
        branch = jnp.dot(act_all[layer], ofull[layer], preferred_element_type=jnp.float32).astype(jnp.bfloat16)
        target[:, half] = (source[:, half].astype(jnp.float32) + branch.astype(jnp.float32)).astype(jnp.bfloat16)
        swap = to_tp(target.at[:, half], target.at[:, half], xsend.at[layer], xrecv.at[layer], partner)
        swap.start()
        tend()
        swap.wait_recv()
        tend()
        if nxt is not None:
            norm_rows(nxt, target)
        tend()
        for copy in copies + stat_copies + [halo_copy]:
            copy.wait_send()
        swap.wait_send()

    for layer in range(layers):
        layer_step(layer, tok_ref if layer == 0 else hid.at[layer - 1], hid.at[layer])
    out_ref[...] = hid[layers - 1]

    doc_copy.wait_send()

    @pl.loop(0, n - 1)
    def _(step):
        for layer in range(layers):
            for msg in range(3):
                for way in range(2):
                    ring_copy(layer, msg, way, step).wait_send()

    @pl.loop(0, n)
    def _(step):
        for layer in range(layers):
            for way in range(2):
                spread(layer, way, step, "wait_send")


def fused_on_device(n, m, tokens, doc_ids, pre_gain, value_proj, gate_proj, out_proj, conv_taps, norm_gain, norm_shift):
    rows, width = tokens.shape
    layers, depth, block = value_proj.shape
    owidth = out_proj.shape[2]
    reach = conv_taps.shape[1] - 1
    channels = block * m
    docs = doc_ids.reshape(rows // 128, 128)
    bf16, f32, i32 = jnp.bfloat16, jnp.float32, jnp.int32
    dma = pltpu.SemaphoreType.DMA
    vmem = pl.BlockSpec(memory_space=pltpu.VMEM)
    return pl.pallas_call(
        functools.partial(fused_kernel, n, m, reach, layers),
        out_shape=jax.ShapeDtypeStruct((rows, width), bf16),
        in_specs=[vmem] * 9,
        out_specs=vmem,
        scratch_shapes=[
            pltpu.VMEM((layers, n * depth, 2 * block), bf16),
            pltpu.VMEM((layers, block, n * owidth), bf16),
            pltpu.VMEM((layers, channels, width // 2), bf16),
            pltpu.VMEM((rows, width), bf16),
            pltpu.VMEM((rows, 2 * block), f32),
            pltpu.VMEM((block // 128 * (rows + HALO), 128), f32),
            pltpu.VMEM((rows + HALO, 128), f32),
            pltpu.VMEM((rows, 128), i32),
            pltpu.VMEM((layers, HALO, block), bf16),
            pltpu.VMEM((layers, HALO, block), bf16),
            pltpu.VMEM((HALO, 128), f32),
            pltpu.VMEM((HALO, 128), f32),
            pltpu.VMEM((rows, 128), f32),
            pltpu.VMEM((layers, 8, rows), f32),
            pltpu.VMEM((layers, m, 8, rows), f32),
            pltpu.VMEM((rows, block), f32),
            pltpu.VMEM((layers, rows, channels), bf16),
            pltpu.VMEM((layers, rows, width), bf16),
            dma((layers, 3, 2, n)), dma((layers, 3, 2, n)),
            dma((layers, 2, n, m // 2)), dma((layers, m, n)),
            dma((layers + 1,)), dma((layers + 1,)),
            dma((layers, m)), dma((layers, m)),
            dma((layers, m)), dma((layers, m)),
            dma((layers,)), dma((layers,)),
        ],
        compiler_params=pltpu.CompilerParams(
            collective_id=0, has_side_effects=True, vmem_limit_bytes=60 * 1024 * 1024),
    )(tokens, docs, pre_gain, value_proj, gate_proj, out_proj, jnp.transpose(conv_taps, (1, 0, 2)), norm_gain, norm_shift)


def passed_along(value, axis, steps):
    count = lax.axis_size(axis)
    first, last = (max(0, -steps), min(count, count - steps))
    return lax.ppermute(value, axis, [(source, source + steps) for source in range(first, last)])


def on_device(
    tokens, doc_ids, pre_gain, value_proj, gate_proj, out_proj, conv_taps, norm_gain, norm_shift
):
    layer_count = value_proj.shape[0]
    tap_count = conv_taps.shape[1]
    reach_rows = tap_count - 1
    row_count = tokens.shape[0]
    block_width = conv_taps.shape[2]
    channels = block_width * lax.axis_size("tp")
    hidden = tokens
    full_value, full_gate, full_out = (
        lax.all_gather(value_proj, "sp", axis=1, tiled=True),
        lax.all_gather(gate_proj, "sp", axis=1, tiled=True),
        lax.all_gather(out_proj, "sp", axis=2, tiled=True),
    )
    for layer_index in range(layer_count):
        wide_state = hidden.astype(jnp.float32)
        scale = lax.rsqrt(jnp.mean(wide_state * wide_state, axis=-1, keepdims=True) + epsilon)
        normed = (wide_state * scale * pre_gain[layer_index]).astype(jnp.bfloat16)
        value_acc = jnp.dot(normed, full_value[layer_index], preferred_element_type=jnp.float32)
        gate_acc = jnp.dot(normed, full_gate[layer_index], preferred_element_type=jnp.float32)
        value_half = value_acc.astype(jnp.bfloat16)
        gate_half = gate_acc.astype(jnp.bfloat16)
        gated_rows = (
            value_half.astype(jnp.float32) * jax.nn.sigmoid(gate_half.astype(jnp.float32))
        ).astype(jnp.bfloat16)
        prev_rows, prev_docs = passed_along(
            (gated_rows[row_count - reach_rows :], doc_ids[row_count - reach_rows :]), "sp", 1
        )
        padded = jnp.concatenate([prev_rows, gated_rows]).astype(jnp.float32)
        padded_docs = jnp.concatenate([prev_docs, doc_ids])
        conv_out = jnp.zeros((row_count, block_width), jnp.float32)
        for offset in range(tap_count):
            first_row = reach_rows - offset
            same_doc = (padded_docs[first_row : first_row + row_count] == doc_ids)[:, None]
            term = (
                conv_taps[layer_index, offset][None, :] * padded[first_row : first_row + row_count]
            )
            conv_out = conv_out + jnp.where(same_doc, term, jnp.float32(0.0))
        row_sums, square_sums = lax.psum(
            (jnp.sum(conv_out, axis=1), jnp.sum(conv_out * conv_out, axis=1)), "tp"
        )
        row_mean = (row_sums / channels)[:, None]
        row_var = (square_sums / channels)[:, None] - row_mean * row_mean
        normalized = (
            norm_gain[layer_index] * (conv_out - row_mean) * lax.rsqrt(row_var + epsilon)
            + norm_shift[layer_index]
        )
        activated = jax.nn.silu(normalized).astype(jnp.bfloat16)
        partial_value = jnp.dot(
            activated, full_out[layer_index], preferred_element_type=jnp.float32
        )
        summed = lax.psum(partial_value.astype(jnp.bfloat16), "tp")
        hidden = (hidden.astype(jnp.float32) + summed.astype(jnp.float32)).astype(jnp.bfloat16)
    return hidden


def suits_kernel(n, m, tokens, value_proj, out_proj, conv_taps):
    rows, width = tokens.shape
    depth, block = value_proj.shape[1:]
    return (
        n % 2 == 0 and 4 <= n <= 16 and m % 2 == 0 and m >= 4 and rows % 128 == 0 and width % 256 == 0
        and depth % 32 == 0 and block % 128 == 0 and out_proj.shape[2] % 256 == 0
        and conv_taps.shape[1] - 1 <= HALO
    )


def solution(mesh):
    n, m = mesh.shape["sp"], mesh.shape["tp"]

    def body(tokens, doc_ids, pre_gain, value_proj, gate_proj, out_proj, conv_taps, norm_gain, norm_shift):
        chosen = on_device
        if suits_kernel(n, m, tokens, value_proj, out_proj, conv_taps):
            chosen = functools.partial(fused_on_device, n, m)
        return chosen(tokens, doc_ids, pre_gain, value_proj, gate_proj, out_proj, conv_taps, norm_gain, norm_shift)

    return jax.shard_map(
        body,
        mesh=mesh,
        in_specs=(
            P("sp", None),
            P("sp"),
            P(),
            P(None, "sp", "tp"),
            P(None, "sp", "tp"),
            P(None, "tp", "sp"),
            P(None, None, "tp"),
            P(None, "tp"),
            P(None, "tp"),
        ),
        out_specs=P("sp", None),
        check_vma=False,
    )
```

```python
import functools
import jax
import jax.numpy as jnp
from jax import lax
from jax.experimental import pallas as pl
from jax.experimental.pallas import tpu as pltpu
from jax.sharding import PartitionSpec as P

epsilon = 1e-06
MESH = pl.DeviceIdType.MESH
HALO = 32
CONV_ROWS = 64


def fused_kernel(
    n, m, reach, layers,
    tok_ref, doc_ref, gain_ref, v_ref, g_ref, o_ref, tap_ref, ng_ref, ns_ref,
    out_ref,
    w, oring, ofull, normed, acc, padded, pdoc, run, ghalo, halo_in, doc_in, doc_tail,
    stat, stat_out, stat_in, conv, act_all, hid,
    rsend, rrecv, osend, orecv, hsend, hrecv, ssend, srecv, asend, arecv, xsend, xrecv,
):
    me = lax.axis_index("sp")
    t = lax.axis_index("tp")
    q, c = t // 2, t % 2
    pairs = m // 2
    half_n = n // 2
    rows, width = tok_ref.shape
    depth, block = v_ref.shape[1], v_ref.shape[2]
    owidth = o_ref.shape[2]
    hd, ho = depth // 2, owidth // 2
    half_width = width // 2
    channels = block * m

    def index_of(position):
        position = (position + 2 * n) % n
        return jnp.where(position < half_n, 2 * position, 2 * (n - 1 - position) + 1)

    my_pos = jnp.where(me % 2 == 0, me // 2, n - 1 - me // 2)
    right, left = index_of(my_pos + 1), index_of(my_pos - 1)
    following, before = (me + 1) % n, (me + n - 1) % n

    barrier = pltpu.get_barrier_semaphore()
    for other in (right, left, following, before):
        pl.semaphore_signal(barrier, inc=1, device_id={"sp": other}, device_id_type=MESH)
    for k in range(1, m):
        pl.semaphore_signal(barrier, inc=1, device_id={"tp": (t + k) % m}, device_id_type=MESH)
    pl.semaphore_wait(barrier, 3 + m)

    def to_sp(src, dst, send, recv, target):
        return pltpu.make_async_remote_copy(
            src_ref=src, dst_ref=dst, send_sem=send, recv_sem=recv,
            device_id={"sp": target}, device_id_type=MESH)

    def to_tp(src, dst, send, recv, target):
        return pltpu.make_async_remote_copy(
            src_ref=src, dst_ref=dst, send_sem=send, recv_sem=recv,
            device_id={"tp": target}, device_id_type=MESH)

    def w_piece(layer, owner, way, part):
        return w.at[layer, pl.ds(pl.multiple_of(owner * depth + part * hd, hd), hd),
                    pl.ds(way * block, block)]

    def o_piece(layer, owner, way):
        return oring.at[layer, :, pl.ds(pl.multiple_of(owner * owidth + way * ho, ho), ho)]

    def ring_copy(layer, msg, way, step, own=False):
        owner = index_of(my_pos - step if way == 0 else my_pos + step)
        if msg < 2:
            dst = w_piece(layer, owner, way, msg)
            src = (v_ref, g_ref)[way].at[layer, pl.ds(msg * hd, hd), :] if own else dst
        else:
            dst = o_piece(layer, owner, way)
            src = o_ref.at[layer, :, pl.ds(way * ho, ho)] if own else dst
        return to_sp(src, dst, rsend.at[layer, msg, way, step], rrecv.at[layer, msg, way, step],
                     right if way == 0 else left)

    def arrival(layer, msg, way, step):
        owner = index_of(my_pos - step - 1 if way == 0 else my_pos + step + 1)
        dst = w_piece(layer, owner, way, msg) if msg < 2 else o_piece(layer, owner, way)
        return to_sp(dst, dst, rsend.at[layer, msg, way, step], rrecv.at[layer, msg, way, step],
                     right if way == 0 else left)

    def spread_copy(layer, way, step, pair, own=False):
        owner = index_of(my_pos - step if way == 0 else my_pos + step)
        part = owner // half_n
        local = owner - part * half_n
        src = o_ref.at[layer, :, pl.ds(way * ho, ho)] if own else o_piece(layer, owner, way)
        dst = ofull.at[layer, pl.ds(pl.multiple_of(t * block, block), block),
                       pl.ds(pl.multiple_of(local * owidth + way * ho, ho), ho)]
        copy = to_tp(src, dst, osend.at[layer, way, step, pair],
                     orecv.at[layer, t, local * 2 + way], 2 * ((q + pair) % pairs) + part)
        return copy, part

    def spread(layer, way, step, act, own=False):
        for pair in range(pairs - 1, -1, -1):
            copy, part = spread_copy(layer, way, step, pair, own)
            if pair == 0:
                pl.when(part != c)(lambda copy=copy: getattr(copy, act)())
            else:
                getattr(copy, act)()

    def slot(time):
        for layer in reversed(range(layers)):
            step = time - (n - 1) * layer
            if not 0 <= step <= n - 1:
                continue
            for msg in range(3):
                for way in range(2):
                    if step > 0:
                        arrival(layer, msg, way, step - 1).wait_recv()
                    if step < n - 1:
                        ring_copy(layer, msg, way, step, own=step == 0).start()
            for way in range(2):
                spread(layer, way, step, "start", own=step == 0)

    def keep_own(layer):
        row = pl.ds(pl.multiple_of(me * depth, depth), depth)
        w[layer, row, pl.ds(0, block)] = v_ref[layer]
        w[layer, row, pl.ds(block, block)] = g_ref[layer]
        oring[layer, :, pl.ds(pl.multiple_of(me * owidth, owidth), owidth)] = o_ref[layer]

    slot(0)

    def doc_block(i):
        row = doc_ref[pl.ds(i, 1), :].astype(jnp.float32)
        return jnp.transpose(jnp.broadcast_to(row, (128, 128)))

    doc_tail[...] = doc_block(rows // 128 - 1)[128 - HALO:]
    doc_copy = to_sp(doc_tail, doc_in, hsend.at[layers],
                     hrecv.at[layers], following)
    doc_copy.start()

    for i in range(rows // 128):
        pdoc[pl.ds(HALO + i * 128, 128), :] = doc_block(i)

    def norm_rows(layer, source):
        @pl.loop(0, rows // 32)
        def _(i):
            span = pl.ds(pl.multiple_of(i * 32, 32), 32)
            wide = source[span, :].astype(jnp.float32)
            scale = lax.rsqrt(jnp.mean(wide * wide, axis=-1, keepdims=True) + epsilon)
            normed[span, :] = (wide * scale * gain_ref[pl.ds(layer, 1), :]).astype(jnp.bfloat16)

    norm_rows(0, tok_ref)
    keep_own(0)
    slot(1)
    doc_copy.wait_recv()
    pdoc[pl.ds(0, HALO), :] = jnp.where(me == 0, jnp.float32(-1.0), doc_in[...])

    @pl.loop(0, rows // CONV_ROWS)
    def _(i):
        base = pl.multiple_of(i * CONV_ROWS, CONV_ROWS)
        mine = pdoc[pl.ds(base + HALO, CONV_ROWS), :]
        count = jnp.zeros((CONV_ROWS, 128), jnp.int32)
        for j in range(1, reach + 1):
            count = count + (pdoc[pl.ds(base + (HALO - j), CONV_ROWS), :] == mine).astype(jnp.int32)
        run[pl.ds(base, CONV_ROWS), :] = count

    for later in range(1, layers):
        keep_own(later)
    for time in range(2, n):
        slot(time)

    lane = lax.broadcasted_iota(jnp.int32, (CONV_ROWS, 128), 1)

    def layer_step(layer, source, target):
        nxt = layer + 1 if layer + 1 < layers else None
        opened = (n - 1) * (layer + 1) + 1
        times = list(range(opened, opened + n - 1)) if nxt is not None else []
        shares = [times[i:i + 1] for i in range(6)] + [times[6:]]

        def tend():
            for time in shares.pop(0):
                slot(time)

        acc[...] = jnp.dot(normed[...], w[layer], preferred_element_type=jnp.float32)

        def store_padded(row, values):
            for part in range(block // 128):
                padded[pl.ds(row + part * (rows + HALO), 32), :] = values[:, part * 128:(part + 1) * 128].astype(jnp.float32)

        def gate_rows(i):
            span = pl.ds(pl.multiple_of(i * 32, 32), 32)
            value = acc[span, pl.ds(0, block)].astype(jnp.bfloat16).astype(jnp.float32)
            gate = acc[span, pl.ds(block, block)].astype(jnp.bfloat16).astype(jnp.float32)
            gated = (value * jax.nn.sigmoid(gate)).astype(jnp.bfloat16)
            store_padded(pl.multiple_of(i * 32 + HALO, 32), gated)
            return gated

        ghalo[layer] = gate_rows(rows // 32 - 1)
        halo_copy = to_sp(ghalo.at[layer], halo_in.at[layer], hsend.at[layer], hrecv.at[layer], following)
        halo_copy.start()

        @pl.loop(0, rows // 32 - 1)
        def _(i):
            gate_rows(i)

        tend()
        halo_copy.wait_recv()
        store_padded(0, halo_in[layer])

        def conv_rows(i):
            base = pl.multiple_of(i * CONV_ROWS, CONV_ROWS)
            count = run[pl.ds(base, CONV_ROWS), :]
            first_sum = jnp.zeros((CONV_ROWS, 1), jnp.float32)
            square_sum = jnp.zeros((CONV_ROWS, 1), jnp.float32)
            for part in range(block // 128):
                cols = pl.ds(part * 128, 128)
                lift = part * (rows + HALO)
                total = tap_ref[0, pl.ds(layer, 1), cols] * padded[pl.ds(base + (lift + HALO), CONV_ROWS), :]
                for j in range(1, reach + 1):
                    term = tap_ref[j, pl.ds(layer, 1), cols] * padded[pl.ds(base + (lift + HALO - j), CONV_ROWS), :]
                    total = total + jnp.where(count >= j, term, jnp.float32(0.0))
                conv[pl.ds(base, CONV_ROWS), cols] = total
                first_sum = first_sum + jnp.sum(total, axis=1, keepdims=True)
                square_sum = square_sum + jnp.sum(total * total, axis=1, keepdims=True)
            stat[pl.ds(base, CONV_ROWS), :] = jnp.where(
                lane == 0, first_sum, jnp.where(lane == 1, square_sum, jnp.float32(0.0)))

        middle = rows // CONV_ROWS // 2
        pl.loop(0, middle)(conv_rows)
        tend()
        pl.loop(middle, rows // CONV_ROWS)(conv_rows)
        stat_out[layer] = jnp.transpose(stat[...])[:8]
        stat_copies = [
            to_tp(stat_out.at[layer], stat_in.at[layer, t], ssend.at[layer, k], srecv.at[layer, t], (t + k) % m)
            for k in range(1, m)]
        for copy in stat_copies:
            copy.start()
        tend()
        summed = stat_out[layer]
        for k in range(1, m):
            peer = (t + k) % m
            to_tp(stat_in.at[layer, peer], stat_in.at[layer, peer], ssend.at[layer, k],
                  srecv.at[layer, peer], peer).wait_recv()
            summed = summed + stat_in[layer, peer]
        stat[...] = jnp.transpose(
            jnp.concatenate([summed, jnp.zeros((120, rows), jnp.float32)], axis=0))

        mine = pl.ds(pl.multiple_of(t * block, block), block)

        @pl.loop(0, rows // CONV_ROWS)
        def _(i):
            span = pl.ds(pl.multiple_of(i * CONV_ROWS, CONV_ROWS), CONV_ROWS)
            both = stat[span, :]
            row_mean = both[:, 0:1] / channels
            row_var = both[:, 1:2] / channels - row_mean * row_mean
            normalized = (ng_ref[pl.ds(layer, 1), :] * (conv[span, :] - row_mean)
                          * lax.rsqrt(row_var + epsilon) + ns_ref[pl.ds(layer, 1), :])
            act_all[layer, span, mine] = jax.nn.silu(normalized).astype(jnp.bfloat16)

        def act_cols(who):
            return act_all.at[layer, :, pl.ds(pl.multiple_of(who * block, block), block)]

        partner = 2 * q + 1 - c
        copies = []
        for k in range(pairs - 1, -1, -1):
            target_t = 2 * ((q + k) % pairs) + c if k else partner
            copies.append(to_tp(act_cols(t), act_cols(t), asend.at[layer, k], arecv.at[layer, t], target_t))
            copies[-1].start()
        tend()
        for k in range(1, pairs):
            sender = 2 * ((q + k) % pairs) + c
            to_tp(act_cols(sender), act_cols(sender), asend.at[layer, k], arecv.at[layer, sender], sender).wait_recv()
            copies.append(to_tp(act_cols(sender), act_cols(sender), asend.at[layer, pairs + k],
                                arecv.at[layer, sender], partner))
            copies[-1].start()
        tend()
        ofull[layer, pl.ds(pl.multiple_of(t * block, block), block), :] = oring[
            layer, :, pl.ds(pl.multiple_of(c * half_width, half_width), half_width)]
        for k in range(1, m):
            peer = (t + k) % m

            @pl.loop(0, n)
            def _(piece, peer=peer):
                dst = ofull.at[layer, pl.ds(pl.multiple_of(peer * block, block), block),
                               pl.ds(pl.multiple_of(piece * ho, ho), ho)]
                to_tp(dst, dst, osend.at[layer, 0, 0, 0], orecv.at[layer, peer, piece], peer).wait_recv()

        for k in range(pairs):
            sender = 2 * ((q + k) % pairs) + 1 - c
            to_tp(act_cols(sender), act_cols(sender), asend.at[layer, k], arecv.at[layer, sender], partner).wait_recv()
        half = pl.ds(pl.multiple_of(c * half_width, half_width), half_width)
        branch = jnp.dot(act_all[layer], ofull[layer], preferred_element_type=jnp.float32).astype(jnp.bfloat16)
        target[:, half] = (source[:, half].astype(jnp.float32) + branch.astype(jnp.float32)).astype(jnp.bfloat16)
        swap = to_tp(target.at[:, half], target.at[:, half], xsend.at[layer], xrecv.at[layer], partner)
        swap.start()
        tend()
        swap.wait_recv()
        if nxt is not None:
            norm_rows(nxt, target)
        tend()
        for copy in copies + stat_copies + [halo_copy]:
            copy.wait_send()
        swap.wait_send()

    for layer in range(layers):
        layer_step(layer, tok_ref if layer == 0 else hid.at[layer - 1], hid.at[layer])
    out_ref[...] = hid[layers - 1]

    doc_copy.wait_send()

    @pl.loop(0, n - 1)
    def _(step):
        for layer in range(layers):
            for msg in range(3):
                for way in range(2):
                    ring_copy(layer, msg, way, step).wait_send()

    @pl.loop(0, n)
    def _(step):
        for layer in range(layers):
            for way in range(2):
                spread(layer, way, step, "wait_send")


def fused_on_device(n, m, tokens, doc_ids, pre_gain, value_proj, gate_proj, out_proj, conv_taps, norm_gain, norm_shift):
    rows, width = tokens.shape
    layers, depth, block = value_proj.shape
    owidth = out_proj.shape[2]
    reach = conv_taps.shape[1] - 1
    channels = block * m
    docs = doc_ids.reshape(rows // 128, 128)
    bf16, f32, i32 = jnp.bfloat16, jnp.float32, jnp.int32
    dma = pltpu.SemaphoreType.DMA
    vmem = pl.BlockSpec(memory_space=pltpu.VMEM)
    return pl.pallas_call(
        functools.partial(fused_kernel, n, m, reach, layers),
        out_shape=jax.ShapeDtypeStruct((rows, width), bf16),
        in_specs=[vmem] * 9,
        out_specs=vmem,
        scratch_shapes=[
            pltpu.VMEM((layers, n * depth, 2 * block), bf16),
            pltpu.VMEM((layers, block, n * owidth), bf16),
            pltpu.VMEM((layers, channels, width // 2), bf16),
            pltpu.VMEM((rows, width), bf16),
            pltpu.VMEM((rows, 2 * block), f32),
            pltpu.VMEM((block // 128 * (rows + HALO), 128), f32),
            pltpu.VMEM((rows + HALO, 128), f32),
            pltpu.VMEM((rows, 128), i32),
            pltpu.VMEM((layers, HALO, block), bf16),
            pltpu.VMEM((layers, HALO, block), bf16),
            pltpu.VMEM((HALO, 128), f32),
            pltpu.VMEM((HALO, 128), f32),
            pltpu.VMEM((rows, 128), f32),
            pltpu.VMEM((layers, 8, rows), f32),
            pltpu.VMEM((layers, m, 8, rows), f32),
            pltpu.VMEM((rows, block), f32),
            pltpu.VMEM((layers, rows, channels), bf16),
            pltpu.VMEM((layers, rows, width), bf16),
            dma((layers, 3, 2, n)), dma((layers, 3, 2, n)),
            dma((layers, 2, n, m // 2)), dma((layers, m, n)),
            dma((layers + 1,)), dma((layers + 1,)),
            dma((layers, m)), dma((layers, m)),
            dma((layers, m)), dma((layers, m)),
            dma((layers,)), dma((layers,)),
        ],
        compiler_params=pltpu.CompilerParams(
            collective_id=0, has_side_effects=True, vmem_limit_bytes=60 * 1024 * 1024),
    )(tokens, docs, pre_gain, value_proj, gate_proj, out_proj, jnp.transpose(conv_taps, (1, 0, 2)), norm_gain, norm_shift)


def passed_along(value, axis, steps):
    count = lax.axis_size(axis)
    first, last = (max(0, -steps), min(count, count - steps))
    return lax.ppermute(value, axis, [(source, source + steps) for source in range(first, last)])


def on_device(
    tokens, doc_ids, pre_gain, value_proj, gate_proj, out_proj, conv_taps, norm_gain, norm_shift
):
    layer_count = value_proj.shape[0]
    tap_count = conv_taps.shape[1]
    reach_rows = tap_count - 1
    row_count = tokens.shape[0]
    block_width = conv_taps.shape[2]
    channels = block_width * lax.axis_size("tp")
    hidden = tokens
    full_value, full_gate, full_out = (
        lax.all_gather(value_proj, "sp", axis=1, tiled=True),
        lax.all_gather(gate_proj, "sp", axis=1, tiled=True),
        lax.all_gather(out_proj, "sp", axis=2, tiled=True),
    )
    for layer_index in range(layer_count):
        wide_state = hidden.astype(jnp.float32)
        scale = lax.rsqrt(jnp.mean(wide_state * wide_state, axis=-1, keepdims=True) + epsilon)
        normed = (wide_state * scale * pre_gain[layer_index]).astype(jnp.bfloat16)
        value_acc = jnp.dot(normed, full_value[layer_index], preferred_element_type=jnp.float32)
        gate_acc = jnp.dot(normed, full_gate[layer_index], preferred_element_type=jnp.float32)
        value_half = value_acc.astype(jnp.bfloat16)
        gate_half = gate_acc.astype(jnp.bfloat16)
        gated_rows = (
            value_half.astype(jnp.float32) * jax.nn.sigmoid(gate_half.astype(jnp.float32))
        ).astype(jnp.bfloat16)
        prev_rows, prev_docs = passed_along(
            (gated_rows[row_count - reach_rows :], doc_ids[row_count - reach_rows :]), "sp", 1
        )
        padded = jnp.concatenate([prev_rows, gated_rows]).astype(jnp.float32)
        padded_docs = jnp.concatenate([prev_docs, doc_ids])
        conv_out = jnp.zeros((row_count, block_width), jnp.float32)
        for offset in range(tap_count):
            first_row = reach_rows - offset
            same_doc = (padded_docs[first_row : first_row + row_count] == doc_ids)[:, None]
            term = (
                conv_taps[layer_index, offset][None, :] * padded[first_row : first_row + row_count]
            )
            conv_out = conv_out + jnp.where(same_doc, term, jnp.float32(0.0))
        row_sums, square_sums = lax.psum(
            (jnp.sum(conv_out, axis=1), jnp.sum(conv_out * conv_out, axis=1)), "tp"
        )
        row_mean = (row_sums / channels)[:, None]
        row_var = (square_sums / channels)[:, None] - row_mean * row_mean
        normalized = (
            norm_gain[layer_index] * (conv_out - row_mean) * lax.rsqrt(row_var + epsilon)
            + norm_shift[layer_index]
        )
        activated = jax.nn.silu(normalized).astype(jnp.bfloat16)
        partial_value = jnp.dot(
            activated, full_out[layer_index], preferred_element_type=jnp.float32
        )
        summed = lax.psum(partial_value.astype(jnp.bfloat16), "tp")
        hidden = (hidden.astype(jnp.float32) + summed.astype(jnp.float32)).astype(jnp.bfloat16)
    return hidden


def suits_kernel(n, m, tokens, value_proj, out_proj, conv_taps):
    rows, width = tokens.shape
    depth, block = value_proj.shape[1:]
    return (
        n % 2 == 0 and 4 <= n <= 16 and m % 2 == 0 and m >= 4 and rows % 128 == 0 and width % 256 == 0
        and depth % 32 == 0 and block % 128 == 0 and out_proj.shape[2] % 256 == 0
        and conv_taps.shape[1] - 1 <= HALO
    )


def solution(mesh):
    n, m = mesh.shape["sp"], mesh.shape["tp"]

    def body(tokens, doc_ids, pre_gain, value_proj, gate_proj, out_proj, conv_taps, norm_gain, norm_shift):
        chosen = on_device
        if suits_kernel(n, m, tokens, value_proj, out_proj, conv_taps):
            chosen = functools.partial(fused_on_device, n, m)
        return chosen(tokens, doc_ids, pre_gain, value_proj, gate_proj, out_proj, conv_taps, norm_gain, norm_shift)

    return jax.shard_map(
        body,
        mesh=mesh,
        in_specs=(
            P("sp", None),
            P("sp"),
            P(),
            P(None, "sp", "tp"),
            P(None, "sp", "tp"),
            P(None, "tp", "sp"),
            P(None, None, "tp"),
            P(None, "tp"),
            P(None, "tp"),
        ),
        out_specs=P("sp", None),
        check_vma=False,
    )
```
